32 devices in a mesh: sp: 16 (over z, y, core), tp: 2 (over x).
Axes of the slice: x: 2, y: 2, z: 4, core: 2. Of those that a mesh axis runs over, the one named last changes fastest.
Arguments:
- tokens: bfloat16 [16384, 2048], P('sp'), may hold values from -6 to 6
- norm_gain: float32 [2048], replicated, may hold values from 0.1 to 1.9
- w_query: bfloat16 [2048, 512], P(None, 'tp'), may hold values from -0.79549513 to 0.79549513
- w_key: bfloat16 [2048, 128], P('sp'), may hold values from -0.79549513 to 0.79549513
- w_value: bfloat16 [2048, 128], P('sp'), may hold values from -0.125 to 0.125
- w_pool_in: bfloat16 [2048, 512], P(None, 'tp'), may hold values from -0.125 to 0.125
- sink_logit: float32 [8], P('tp'), may hold values from 3 to 7
- pool_scale: float32 [512], P('tp'), may hold values from 0.05 to 0.5
- w_out: bfloat16 [1024, 2048], P('tp', 'sp'), may hold values from -0.75 to 0.75
Outputs:
- mixed_out: bfloat16 [16384, 2048], P(('sp', 'tp'))
The draws below stay inside these ranges and needn't reach their ends.
All inputs are finite; a program needn't handle non-finite values.
Results may differ from the reference program's by a relative error of at most 0.03.
The reference program's roundings to bfloat16 on the way (of `normed`, `query`, `key`, `value`, `pool_in`, `weights`, `attended` and `pooled`) count: a program that leaves them out, or rounds other values in their place, can miss the bound.
Values may be sent and summed in bfloat16 or wider, within the bound.
No kernel may reach another device: no remote copies, remote signals or barrier semaphores. Data moves between devices by JAX's collectives and lax.ppermute only.
A program may use at most 64 MiB of HBM per device.

```python
import math
import jax
import jax.numpy as jnp
from jax import lax

D = 2048
HEAD = 64
QH = 8
KVH = 2
POOL_CH = 128
POOL_W = 512
WINDOW = 128
QB = 128
SEQ = 16384


def projection_draw(key, shape):
    values = jax.random.truncated_normal(key, -6.0, 6.0, shape, jnp.float32) * D ** (-0.5)
    return values.astype(jnp.bfloat16)


def draw_w_query(key, part):
    return projection_draw(jax.random.fold_in(key, 11), (D, QH * HEAD))


def draw_w_key(key, part):
    return projection_draw(jax.random.fold_in(key, 23), (D, KVH * HEAD))


def level_of(key, dims, pieces, smallest, top_value):
    level = 1.0
    for dim, parts in pieces:
        steps = jax.random.uniform(jax.random.fold_in(jax.random.fold_in(key, 6), dim), (parts,), jnp.float32, smallest / len(pieces), top_value / len(pieces))
        level = level * jnp.repeat(jnp.exp(steps), dims[dim] // parts).reshape((-1,) + (1,) * (len(dims) - 1 - dim))
    return level


def centred(rng, dims, scale, reach, pieces=(), kind=jnp.bfloat16):
    entries = scale * jax.random.normal(rng, dims, jnp.float32)
    if pieces:
        entries = entries * level_of(rng, dims, pieces, -0.22, 0.18)
    return jnp.clip(entries, -reach, reach).astype(kind)


def setup_inputs(seed: int = 0) -> dict:
    seeds = jax.random.split(jax.random.key(seed), 10)
    tokens = centred(seeds[0], (SEQ, D), 1.0, 6.0, ((0, 16),))
    norm_gain = jnp.clip(1.0 + 0.18 * jax.random.normal(seeds[1], (D,), jnp.float32), 0.1, 1.9)
    w_query = draw_w_query(jax.random.fold_in(seeds[9], 71), 0)
    w_key = draw_w_key(jax.random.fold_in(seeds[9], 71), 0)
    w_value = centred(seeds[4], (D, KVH * HEAD), D ** -0.5, 0.125, ((0, 16),))
    w_pool_in = centred(seeds[5], (D, POOL_W), D ** -0.5, 0.125, ((1, 2),))
    sink_logit = jnp.clip(3.0 + 4.0 * jax.random.uniform(seeds[6], (QH,), jnp.float32) ** level_of(seeds[6], (QH,), ((0, 2),), -0.2, 0.2), 3.0, 7.0)
    pool_scale = jnp.clip(jnp.exp(math.log(0.5) - 2.3025851 * jax.random.uniform(seeds[7], (POOL_W,), jnp.float32) ** level_of(seeds[7], (POOL_W,), ((0, 2),), -0.2, 0.2)), 0.05, 0.5)
    w_out = centred(seeds[8], (QH * HEAD + POOL_W, D), (4.0 * (QH * HEAD + POOL_W) ** -0.5), 0.75, ((0, 2), (1, 16)))
    return {"tokens": tokens, "norm_gain": norm_gain, "w_query": w_query, "w_key": w_key, "w_value": w_value, "w_pool_in": w_pool_in, "sink_logit": sink_logit, "pool_scale": pool_scale, "w_out": w_out}


NEG_BIG = -1e+30
POOL_SPANS = (2, 4, 8, 16)

def layer_normed(tokens, norm_gain):
    values = tokens.astype(jnp.float32)
    center = lax.optimization_barrier(jnp.mean(values, axis=-1, keepdims=True))
    spread = lax.optimization_barrier(jnp.mean(jnp.square(values - center), axis=-1, keepdims=True))
    return ((values - center) * lax.rsqrt(spread + 1e-06) * norm_gain).astype(jnp.bfloat16)

def rotate(values, positions):
    half = HEAD // 2
    inverse = 10000.0 ** (-jnp.arange(half, dtype=jnp.float32) / half)
    angles = positions[:, None] * inverse[None, :]
    cosine = jnp.cos(angles)[:, None, :]
    sine = jnp.sin(angles)[:, None, :]
    first = values[..., :half]
    second = values[..., half:]
    return jnp.concatenate([first * cosine - second * sine, first * sine + second * cosine], axis=-1)

def reference(tokens, norm_gain, w_query, w_key, w_value, w_pool_in, sink_logit, pool_scale, w_out):
    length = tokens.shape[0]
    group = QH // KVH
    normed = layer_normed(tokens, norm_gain)
    positions = jnp.arange(length).astype(jnp.float32)
    query = rotate(jnp.dot(normed, w_query, preferred_element_type=jnp.float32).reshape(length, QH, HEAD), positions).astype(jnp.bfloat16)
    key = rotate(jnp.dot(normed, w_key, preferred_element_type=jnp.float32).reshape(length, KVH, HEAD), positions).astype(jnp.bfloat16)
    value = jnp.dot(normed, w_value, preferred_element_type=jnp.float32).astype(jnp.bfloat16).reshape(length, KVH, HEAD)
    pool_in = jnp.dot(normed, w_pool_in, preferred_element_type=jnp.float32).astype(jnp.bfloat16)
    key_padded = jnp.pad(key, ((WINDOW, WINDOW), (0, 0), (0, 0)))
    value_padded = jnp.pad(value, ((WINDOW, WINDOW), (0, 0), (0, 0)))
    span = QB + 2 * WINDOW
    sink_grid = sink_logit.reshape(KVH, group)[:, :, None, None]

    def attend(start):
        queries = lax.dynamic_slice_in_dim(query, start, QB, 0).reshape(QB, KVH, group, HEAD)
        keys = lax.dynamic_slice_in_dim(key_padded, start, span, 0)
        values = lax.dynamic_slice_in_dim(value_padded, start, span, 0)
        scores = jnp.einsum('ikgd,jkd->kgij', queries.astype(jnp.float32), keys.astype(jnp.float32)) * HEAD ** (-0.5)
        query_pos = start + jnp.arange(QB).astype(jnp.int32)
        key_pos = start - WINDOW + jnp.arange(span).astype(jnp.int32)
        valid = (jnp.abs(query_pos[:, None] - key_pos[None, :]) <= WINDOW) & (key_pos[None, :] >= 0) & (key_pos[None, :] < length)
        scores = jnp.where(valid, scores, NEG_BIG)
        highest = jnp.maximum(lax.optimization_barrier(jnp.max(scores, axis=-1, keepdims=True)), sink_grid)
        expo = jnp.where(valid, jnp.exp(scores - highest), 0.0)
        total = lax.optimization_barrier(jnp.sum(expo, axis=-1, keepdims=True)) + jnp.exp(sink_grid - highest)
        weights = (expo / total).astype(jnp.bfloat16)
        result = jnp.einsum('kgij,jkd->ikgd', weights.astype(jnp.float32), values.astype(jnp.float32))
        return result.reshape(QB, QH * HEAD).astype(jnp.bfloat16)
    starts = (jnp.arange(length // QB) * QB).astype(jnp.int32)
    attended = lax.map(attend, starts).reshape(length, QH * HEAD)
    pool_vals = pool_in.astype(jnp.float32)
    running = jnp.pad(jnp.cumsum(pool_vals, axis=0), ((1, 0), (0, 0)))
    where_at = jnp.arange(length).astype(jnp.int32)
    means = []
    for index, width in enumerate(POOL_SPANS):
        lower = jnp.clip(where_at - width // 2, 0, length)
        upper = jnp.clip(where_at + width // 2, 0, length)
        block = running[:, index * POOL_CH:(index + 1) * POOL_CH]
        means.append((block[upper] - block[lower]) / (upper - lower).astype(jnp.float32)[:, None])
    pooled = ((jnp.concatenate(means, axis=1) - pool_vals) * pool_scale).astype(jnp.bfloat16)
    joined = jnp.concatenate([attended, pooled], axis=1)
    return jnp.dot(joined, w_out, preferred_element_type=jnp.float32).astype(jnp.bfloat16)
```

```python
import functools

import jax
import jax.numpy as jnp
import numpy as np
from jax import lax
from jax.experimental import pallas as pl
from jax.experimental.pallas import tpu as pltpu
from jax.sharding import PartitionSpec as P

HEAD = 64
QH = 8
KVH = 2
POOL_CH = 128
WINDOW = 128
QB = 128


NEG_BIG = -1e30
POOL_SPANS = (2, 4, 8, 16)


def extended(block, sides, width):
    for axis, dim in sides:
        count = lax.axis_size(axis)
        forward = [(i, i + 1) for i in range(count - 1)]
        backward = [(target, source) for source, target in forward]
        low = lax.ppermute(
            lax.slice_in_dim(block, block.shape[dim] - width, None, axis=dim), axis, forward
        )
        high = lax.ppermute(lax.slice_in_dim(block, 0, width, axis=dim), axis, backward)
        block = jnp.concatenate([low, block, high], axis=dim)
    return block


def layer_normed(tokens, norm_gain):
    values = tokens.astype(jnp.float32)
    center = jnp.mean(values, axis=-1, keepdims=True)
    spread = jnp.mean(jnp.square(values - center), axis=-1, keepdims=True)
    return ((values - center) * lax.rsqrt(spread + 1e-06) * norm_gain).astype(jnp.bfloat16)


def rotate(values, positions):
    half = HEAD // 2
    inverse = 10000.0 ** (-jnp.arange(half, dtype=jnp.float32) / half)
    angles = positions[:, None] * inverse[None, :]
    cosine = jnp.cos(angles)[:, None, :]
    sine = jnp.sin(angles)[:, None, :]
    first = values[..., :half]
    second = values[..., half:]
    return jnp.concatenate(
        [first * cosine - second * sine, first * sine + second * cosine], axis=-1
    )


def plain_body(tokens, norm_gain, w_query, w_key, w_value, w_pool_in, sink_logit, pool_scale, w_out):
    local_rows = tokens.shape[0]
    seq_total = local_rows * lax.axis_size("sp")
    offset = lax.axis_index("sp") * local_rows
    tp_place = lax.axis_index("tp")
    local_heads = w_query.shape[1] // HEAD
    local_pool = w_pool_in.shape[1]
    reach = POOL_SPANS[-1] // 2
    normed = layer_normed(tokens, norm_gain)
    positions = (offset + jnp.arange(local_rows)).astype(jnp.float32)
    query = rotate(
        jnp.dot(normed, w_query, preferred_element_type=jnp.float32).reshape(
            local_rows, local_heads, HEAD
        ),
        positions,
    ).astype(jnp.bfloat16)
    key_head = tp_place * local_heads // (QH // KVH)
    key_cols = lax.dynamic_slice_in_dim(w_key, key_head * HEAD, HEAD, 1)
    value_cols = lax.dynamic_slice_in_dim(w_value, key_head * HEAD, HEAD, 1)
    key_sum = jnp.dot(
        normed,
        lax.all_gather(key_cols, "sp", axis=0, tiled=True),
        preferred_element_type=jnp.float32,
    )
    value_sum = jnp.dot(
        normed,
        lax.all_gather(value_cols, "sp", axis=0, tiled=True),
        preferred_element_type=jnp.float32,
    )
    key = rotate(key_sum[:, None, :], positions)[:, 0, :].astype(jnp.bfloat16)
    value = value_sum.astype(jnp.bfloat16)
    key_value = jnp.concatenate([key, value], axis=1)
    pool_in = jnp.dot(normed, w_pool_in, preferred_element_type=jnp.float32).astype(jnp.bfloat16)
    widened = extended(jnp.concatenate([key_value, pool_in], axis=1), (("sp", 0),), WINDOW)
    kv_wide = widened[:, : 2 * HEAD]
    pool_wide = widened[WINDOW - reach : WINDOW + local_rows + reach, 2 * HEAD :]
    span = QB + 2 * WINDOW
    sink_here = sink_logit[:, None, None]
    results = []
    for block in range(local_rows // QB):
        queries = query[block * QB : (block + 1) * QB]
        keys = kv_wide[block * QB : block * QB + span, :HEAD]
        values = kv_wide[block * QB : block * QB + span, HEAD:]
        scores = jnp.einsum(
            "ihd,jd->hij", queries, keys, preferred_element_type=jnp.float32
        ) * HEAD ** (-0.5)
        query_pos = offset + block * QB + jnp.arange(QB)
        key_pos = offset + block * QB - WINDOW + jnp.arange(span)
        valid = (
            (jnp.abs(query_pos[:, None] - key_pos[None, :]) <= WINDOW)
            & (key_pos[None, :] >= 0)
            & (key_pos[None, :] < seq_total)
        )
        scores = jnp.where(valid, scores, NEG_BIG)
        highest = jnp.maximum(jnp.max(scores, axis=-1, keepdims=True), sink_here)
        expo = jnp.where(valid, jnp.exp(scores - highest), 0.0)
        total = jnp.sum(expo, axis=-1, keepdims=True) + jnp.exp(sink_here - highest)
        weights = (expo / total).astype(jnp.bfloat16)
        result = jnp.einsum("hij,jd->ihd", weights, values, preferred_element_type=jnp.float32)
        results.append(result.reshape(QB, local_heads * HEAD).astype(jnp.bfloat16))
    attended = jnp.concatenate(results, axis=0)
    pool_vals = pool_wide.astype(jnp.float32)
    window_sum = pool_vals
    global_pos = offset + jnp.arange(local_rows)
    channel = tp_place * local_pool + jnp.arange(local_pool)
    window_group = channel // POOL_CH
    measured = jnp.zeros((local_rows, local_pool), jnp.float32)
    stride = 1
    for index, width in enumerate(POOL_SPANS):
        window_sum = window_sum[:-stride] + window_sum[stride:]
        stride = width
        sums = window_sum[reach - width // 2 : reach - width // 2 + local_rows]
        counted = (
            jnp.minimum(global_pos + width // 2, seq_total)
            - jnp.maximum(global_pos - width // 2, 0)
        ).astype(jnp.float32)
        measured = measured + jnp.where(
            window_group[None, :] == index, sums / counted[:, None], 0.0
        )
    pooled = ((measured - pool_vals[reach : reach + local_rows]) * pool_scale).astype(jnp.bfloat16)
    attended_rows, pooled_rows = (
        lax.all_to_all(attended, "tp", split_axis=0, concat_axis=1, tiled=True),
        lax.all_to_all(pooled, "tp", split_axis=0, concat_axis=1, tiled=True),
    )
    joined = jnp.concatenate([attended_rows, pooled_rows], axis=1)
    out_rows_all = lax.all_gather(w_out, "tp", axis=0, tiled=True)
    projected = jnp.dot(
        joined,
        lax.all_gather(out_rows_all, "sp", axis=1, tiled=True),
        preferred_element_type=jnp.float32,
    )
    return projected.astype(jnp.bfloat16)


LANES = 128
ROW_TILE = 256
BF16 = jnp.bfloat16
F32 = jnp.float32


def whole():
    return pl.BlockSpec(memory_space=pltpu.VMEM)


def scalars():
    return pl.BlockSpec(memory_space=pltpu.SMEM)


def aligned(start, size=QB):
    return pl.ds(pl.multiple_of(start, QB), size)


def cost(flops, moved=0):
    return pl.CostEstimate(flops=flops, bytes_accessed=moved, transcendentals=0)


def rope_lanes(values, cosine, sine):
    lane = lax.broadcasted_iota(jnp.int32, values.shape, 1)
    swapped = jnp.where(
        lane % HEAD < HEAD // 2,
        pltpu.roll(values, LANES - HEAD // 2, 1),
        pltpu.roll(values, HEAD // 2, 1),
    )
    return values * cosine + swapped * sine


def project_kernel(tokens, gain, w_query, w_pool, cosine, sine, normed, query, pool):
    for row in range(0, tokens.shape[0], 16):
        rows = slice(row, row + 16)
        values = tokens[rows, :].astype(F32)
        centred = values - jnp.mean(values, axis=-1, keepdims=True)
        spread = jnp.mean(centred * centred, axis=-1, keepdims=True)
        normed[rows, :] = (centred * lax.rsqrt(spread + 1e-06) * gain[...]).astype(BF16)
    left = normed[...]
    pool[...] = jnp.dot(left, w_pool[...], preferred_element_type=F32).astype(BF16)
    products = jnp.dot(left, w_query[...], preferred_element_type=F32)
    for lane in range(0, products.shape[1], LANES):
        turned = rope_lanes(products[:, lane : lane + LANES], cosine[...], sine[...])
        query[:, lane : lane + LANES] = turned.astype(BF16) * HEAD ** (-0.5)


def key_value_kernel(places, normed, *refs):
    pieces, (cosine, sine, pool_head, pool_tail, key_value, head, tail, weight) = refs[:4], refs[4:]
    step, last = pl.program_id(0), pl.num_programs(0) - 1
    depth = pieces[0].shape[1]

    @pl.when(step == 0)
    def _():
        for index, piece in enumerate(pieces):
            for slot in range(piece.shape[0]):
                place = places[index * piece.shape[0] + slot]
                weight[pl.ds(pl.multiple_of(place * depth, depth), depth), :] = piece[slot]

    products = jnp.dot(normed[...], weight[...], preferred_element_type=F32)
    lane = lax.broadcasted_iota(jnp.int32, products.shape, 1)
    turned = rope_lanes(products, cosine[...], sine[...])
    result = jnp.where(lane < HEAD, turned, products).astype(BF16)
    key_value[...] = result
    edge = pool_head.shape[0]
    for when, out, rows, pool in (
        (step == 0, head, result[:WINDOW], pool_head),
        (step == last, tail, result[-WINDOW:], pool_tail),
    ):

        @pl.when(when)
        def _(out=out, rows=rows, pool=pool):
            out[:WINDOW, :] = rows
            for group in range(pool.shape[1] // LANES):
                start = WINDOW + group * edge
                out[start : start + edge, :] = pool[:, group * LANES : (group + 1) * LANES]


def pool_kernel(info, pool, low, high, scale, out, wide):
    rows, channels = pool.shape
    edge = (wide.shape[0] - rows) // 2
    chunks, chunk = out.shape[0], out.shape[1]
    place, total = info[0], info[2] * rows
    tp = info[1]
    groups = channels // LANES
    for group in range(groups):
        start = WINDOW + group * edge
        lanes = slice(group * LANES, (group + 1) * LANES)
        wide[:edge, lanes] = low[start : start + edge, :]
        wide[edge + rows :, lanes] = high[start : start + edge, :]
    wide[edge : edge + rows, :] = pool[...]
    span = QB + 2 * edge
    row = lax.broadcasted_iota(jnp.int32, (QB, span), 0) + edge
    column = lax.broadcasted_iota(jnp.int32, (QB, span), 1)
    bands, reaches = [], []
    for group in range(groups):
        reach = lax.shift_left(jnp.int32(1), tp * groups + group)
        inside = (column >= row - reach) & (column < row + reach)
        bands.append(jnp.where(inside, 1.0, 0.0).astype(BF16))
        reaches.append(reach)
    for step in range(chunks):
        target = lax.bitwise_xor(tp, step)
        for block in range(0, chunk, QB):
            start = target * chunk + block
            position = place * rows + start + lax.broadcasted_iota(jnp.int32, (QB, 1), 0)
            for group in range(groups):
                lanes = slice(group * LANES, (group + 1) * LANES)
                sums = jnp.dot(
                    bands[group],
                    wide[aligned(start, span), lanes],
                    preferred_element_type=F32,
                )
                counted = jnp.minimum(position + reaches[group], total) - jnp.maximum(
                    position - reaches[group], 0
                )
                mean = sums * (1.0 / counted.astype(F32))
                own = pool[aligned(start), lanes].astype(F32)
                out[step, block : block + QB, lanes] = ((mean - own) * scale[:, lanes]).astype(BF16)


def attend_kernel(step, info, sink, query, key_value, low, high, out, keys, values):
    chunk = out.shape[0]
    place, tp, count = info[0], info[1], info[2]
    target = lax.bitwise_xor(tp, step)
    chunks = query.shape[0] // chunk
    begin = pl.multiple_of(target * chunk, chunk)

    def put(start, rows):
        wide = rows.astype(F32)
        lane = lax.broadcasted_iota(jnp.int32, wide.shape, 1)
        turned = pltpu.roll(wide, HEAD, 1)
        for side, (key, value) in enumerate(((wide, turned), (turned, wide))):
            first = lane < HEAD if side == 0 else lane >= HEAD
            keys[side, start : start + rows.shape[0], :] = jnp.where(first, key, 0.0).astype(BF16)
            values[side, start : start + rows.shape[0], :] = jnp.where(first, value, 0.0).astype(
                BF16
            )

    for block in range(0, chunk, QB):
        put(WINDOW + block, key_value[aligned(begin + block), :])
    before = key_value[aligned(jnp.maximum(begin - WINDOW, 0)), :]
    put(0, jnp.where(target == 0, low[:WINDOW, :], before))
    after_start = jnp.minimum(begin + chunk, query.shape[0] - WINDOW)
    after = key_value[aligned(after_start), :]
    put(WINDOW + chunk, jnp.where(target == chunks - 1, high[:WINDOW, :], after))

    row = lax.broadcasted_iota(jnp.int32, (QB, WINDOW), 0)
    column = lax.broadcasted_iota(jnp.int32, (QB, WINDOW), 1)
    at_start = (place == 0) & (target == 0)
    at_end = (place == count - 1) & (target == chunks - 1)
    for block in range(0, chunk, QB):
        low_ok, high_ok = column >= row, column <= row
        if block == 0:
            low_ok = low_ok & jnp.logical_not(at_start)
        if block == chunk - QB:
            high_ok = high_ok & jnp.logical_not(at_end)
        for pair in range(query.shape[1] // LANES):
            lanes = slice(pair * LANES, (pair + 1) * LANES)
            queries = query[aligned(begin + block), lanes]
            result = None
            for side in range(2):
                scores = lax.dot_general(
                    queries,
                    keys[side, block : block + QB + 2 * WINDOW, :],
                    (((1,), (1,)), ((), ())),
                    preferred_element_type=F32,
                )
                parts = (
                    jnp.where(low_ok, scores[:, :WINDOW], NEG_BIG),
                    scores[:, WINDOW : WINDOW + QB],
                    jnp.where(high_ok, scores[:, WINDOW + QB :], NEG_BIG),
                )
                logit = sink[2 * pair + side]
                top = jnp.maximum(jnp.maximum(parts[0], parts[1]), parts[2])
                top = jnp.maximum(jnp.max(top, axis=-1, keepdims=True), logit)
                expo = [jnp.exp(part - top) for part in parts]
                total = jnp.sum(expo[0] + expo[1] + expo[2], axis=-1, keepdims=True)
                inverse = 1.0 / (total + jnp.exp(logit - top))
                weights = jnp.concatenate([(part * inverse).astype(BF16) for part in expo], axis=1)
                part = jnp.dot(
                    weights,
                    values[side, block : block + QB + 2 * WINDOW, :],
                    preferred_element_type=F32,
                )
                result = part if result is None else result + part
            out[block : block + QB, lanes] = result.astype(BF16)


def output_kernel(parts, table, info, *refs):
    attended, pooled = refs[:parts], refs[parts : 2 * parts]
    sources, out = refs[2 * parts : 2 * parts + 4], refs[2 * parts + 4]
    weight, joined, staged, in_sem, out_sem = refs[2 * parts + 5 :]
    loads = [
        pltpu.make_async_copy(source, weight.at[index], in_sem.at[index])
        for index, source in enumerate(sources)
    ]
    order = (0, 2, 1, 3)
    for index in order:
        loads[index].start()
    tp = info[1]
    width = attended[0].shape[1]
    for step in range(parts):
        owner = lax.bitwise_xor(tp, step)
        for half, part in enumerate((attended[step], pooled[step])):
            start = pl.multiple_of((half * parts + owner) * width, LANES)
            joined[:, pl.ds(start, width)] = part[...]
    depth, lanes = weight.shape[2], weight.shape[3]
    blocks = weight.shape[1] // parts
    stores = []
    for index in order:
        loads[index].wait()
        for block in range(0, blocks, 2):
            total = None
            entries = [(index * blocks + block + side) * (parts + 1) for side in range(2)]
            for step in range(parts):
                start = pl.multiple_of(lax.bitwise_xor(tp, step) * depth, LANES)
                right = jnp.concatenate(
                    [weight[index, table[entry + 1 + step]] for entry in entries], axis=1
                )
                product = jnp.dot(
                    joined[:, pl.ds(start, depth)], right, preferred_element_type=F32
                )
                total = product if total is None else total + product
            for side in range(2):
                number = index * blocks + block + side
                staged[number] = total[:, side * lanes : (side + 1) * lanes].astype(BF16)
                start = pl.multiple_of(table[entries[side]] * lanes, LANES)
                store = pltpu.make_async_copy(
                    staged.at[number], out.at[:, pl.ds(start, lanes)], out_sem.at[number]
                )
                store.start()
                stores.append(store)
    for store in stores:
        store.wait()


def exchange_orders(sp_count, tp_count):
    sp_bits = [tp_count << bit for bit in range(1, sp_count.bit_length() - 1)][::-1]
    tp_bits = [1 << bit for bit in range(tp_count.bit_length() - 1)]
    for bits in (sp_bits, sp_bits[:1] + tp_bits + sp_bits[1:]):
        yield bits, bits[-1:] + bits[:-1]


def slot_masks(bits):
    masks = [0]
    for bit in bits:
        masks = masks + [mask ^ bit for mask in masks]
    return masks


def doubled(block, orders, sp_count, tp_count):
    even, odd = orders
    devices = range(sp_count * tp_count)

    def send(array, masks):
        pairs = [(i, i ^ masks[(i // tp_count) & 1]) for i in devices]
        return lax.ppermute(array, ("sp", "tp"), pairs)

    held = block[None]
    for masks in zip(even[:-1], odd[:-1]):
        held = jnp.concatenate([held, send(held, masks)], axis=0)
    core = (tp_count, tp_count)
    other = send(held, core)
    came = send(held, (even[-1], odd[-1]))
    return held, came, other, send(came, core)


def fast_body(tokens, norm_gain, w_query, w_key, w_value, w_pool_in, sink_logit, pool_scale, w_out):
    sp_count, tp_count = lax.axis_size("sp"), lax.axis_size("tp")
    local_rows, width = tokens.shape
    sp_place, tp_place = lax.axis_index("sp"), lax.axis_index("tp")
    local_heads = w_query.shape[1] // HEAD
    heads_width, local_pool = w_query.shape[1], w_pool_in.shape[1]
    chunk = local_rows // tp_count
    kv_orders, out_orders = exchange_orders(sp_count, tp_count)

    key_head = tp_place * local_heads // (QH // KVH)
    kv_block = jnp.concatenate(
        [lax.dynamic_slice_in_dim(w, key_head * HEAD, HEAD, 1) for w in (w_key, w_value)], axis=1
    )
    kv_pieces = doubled(kv_block, kv_orders, sp_count, tp_count)
    out_pieces = doubled(w_out, out_orders, sp_count, tp_count)

    odd = sp_place % 2
    info = jnp.stack([sp_place, tp_place, jnp.int32(sp_count)]).astype(jnp.int32)

    def by_class(pairs):
        return jnp.where(odd == 0, jnp.array(pairs[0], jnp.int32), jnp.array(pairs[1], jnp.int32))

    kv_tables, out_tables = [], []
    for flip in range(2):
        for late in range(2):
            rows = []
            for order in (kv_orders if flip == 0 else kv_orders[::-1]):
                extra = order[-1] if late else 0
                rows.append([((mask ^ extra) // tp_count) ^ flip for mask in slot_masks(order[:-1])])
            kv_tables.append(by_class(rows) ^ sp_place)
            rows = []
            for order in (out_orders if flip == 0 else out_orders[::-1]):
                extra = order[-1] if late else 0
                masks = [mask ^ extra for mask in slot_masks(order[:-1])]
                found = {}
                for slot, mask in enumerate(masks):
                    found.setdefault(mask // tp_count, {})[mask % tp_count] = slot
                rows.append(
                    [[delta ^ flip] + [slots[t] for t in range(tp_count)] for delta, slots in found.items()]
                )
            picked = by_class(rows)
            out_tables.append(picked ^ jnp.pad(sp_place[None], (0, tp_count))[None, :])
    kv_table = jnp.concatenate(kv_tables)
    out_table = jnp.concatenate(out_tables).reshape(-1)

    half = HEAD // 2
    inverse = 10000.0 ** (-jnp.arange(half, dtype=F32) / half)
    inverse = jnp.tile(inverse, LANES // half)
    positions = (sp_place * local_rows + jnp.arange(local_rows)).astype(F32)
    angles = positions[:, None] * inverse[None, :]
    cosine = jnp.cos(angles)
    sign = jnp.where(jnp.arange(LANES) % HEAD < half, -1.0, 1.0).astype(F32)
    sine = jnp.sin(angles) * sign[None, :]

    def rows_of(columns, size=ROW_TILE):
        return pl.BlockSpec((size, columns), lambda i: (i, 0))

    def fixed(shape, index=0):
        return pl.BlockSpec(shape, lambda i: (index,) + (0,) * (len(shape) - 1))

    tiles = local_rows // ROW_TILE
    normed, query, pool_in = pl.pallas_call(
        project_kernel,
        grid=(tiles,),
        in_specs=[
            rows_of(width),
            fixed((1, width)),
            fixed(w_query.shape),
            fixed(w_pool_in.shape),
            rows_of(LANES),
            rows_of(LANES),
        ],
        out_specs=[rows_of(width), rows_of(heads_width), rows_of(local_pool)],
        out_shape=[
            jax.ShapeDtypeStruct(tokens.shape, BF16),
            jax.ShapeDtypeStruct((local_rows, heads_width), BF16),
            jax.ShapeDtypeStruct((local_rows, local_pool), BF16),
        ],
        cost_estimate=cost(2 * local_rows * width * (heads_width + local_pool)),
        name="project",
    )(tokens, norm_gain[None, :], w_query, w_pool_in, cosine, sine)

    edge = 2 * (POOL_SPANS[-1] // 2)
    payload = (WINDOW + edge * (local_pool // LANES), LANES)
    key_value, head, tail = pl.pallas_call(
        key_value_kernel,
        grid=(tiles,),
        in_specs=[scalars(), rows_of(width)]
        + [fixed(piece.shape) for piece in kv_pieces]
        + [
            rows_of(LANES),
            rows_of(LANES),
            fixed((edge, local_pool)),
            fixed((edge, local_pool), local_rows // edge - 1),
        ],
        out_specs=[rows_of(LANES), fixed(payload), fixed(payload)],
        out_shape=[
            jax.ShapeDtypeStruct((local_rows, LANES), BF16),
            jax.ShapeDtypeStruct(payload, BF16),
            jax.ShapeDtypeStruct(payload, BF16),
        ],
        scratch_shapes=[pltpu.VMEM((width, LANES), BF16)],
        cost_estimate=cost(2 * local_rows * width * LANES),
        name="key_value",
    )(kv_table, normed, *kv_pieces, cosine, sine, pool_in, pool_in)

    forward = [(i, i + 1) for i in range(sp_count - 1)]
    low = lax.ppermute(tail, "sp", forward)
    high = lax.ppermute(head, "sp", [(target, source) for source, target in forward])

    pooled = pl.pallas_call(
        pool_kernel,
        in_specs=[scalars()] + [whole()] * 4,
        out_specs=whole(),
        out_shape=jax.ShapeDtypeStruct((tp_count, chunk, local_pool), BF16),
        scratch_shapes=[pltpu.VMEM((local_rows + 2 * edge, local_pool), BF16)],
        cost_estimate=cost(2 * local_rows * local_pool * 160),
        name="pool",
    )(info, pool_in, low, high, pool_scale[None, :])

    devices = range(tp_count)

    def hand_over(part, step):
        if step == 0:
            return part
        return lax.ppermute(part, "tp", [(i, i ^ step) for i in devices])

    pooled_parts = [hand_over(pooled[step], step) for step in devices]

    attended_parts = [None] * tp_count
    for step in list(devices)[1:] + [0]:
        attended = pl.pallas_call(
            functools.partial(attend_kernel, step),
            in_specs=[scalars(), scalars()] + [whole()] * 4,
            out_specs=whole(),
            out_shape=jax.ShapeDtypeStruct((chunk, heads_width), BF16),
            scratch_shapes=[pltpu.VMEM((2, chunk + 2 * WINDOW, LANES), BF16)] * 2,
            cost_estimate=cost(4 * chunk * 3 * WINDOW * LANES * local_heads),
            name=f"attend{step}",
        )(info, sink_logit, query, key_value, low, high)
        attended_parts[step] = hand_over(attended, step)

    columns = w_out.shape[1] * sp_count
    return pl.pallas_call(
        functools.partial(output_kernel, tp_count),
        in_specs=[scalars(), scalars()]
        + [whole()] * (2 * tp_count)
        + [pl.BlockSpec(memory_space=pltpu.HBM)] * 4,
        out_specs=pl.BlockSpec(memory_space=pltpu.HBM),
        out_shape=jax.ShapeDtypeStruct((chunk, columns), BF16),
        scratch_shapes=[
            pltpu.VMEM((4,) + out_pieces[0].shape, BF16),
            pltpu.VMEM((chunk, w_out.shape[0] * tp_count), BF16),
            pltpu.VMEM((sp_count, chunk, w_out.shape[1]), BF16),
            pltpu.SemaphoreType.DMA((4,)),
            pltpu.SemaphoreType.DMA((sp_count,)),
        ],
        cost_estimate=cost(2 * chunk * columns * w_out.shape[0] * tp_count),
        name="output",
    )(out_table, info, *attended_parts, *pooled_parts, *out_pieces)


def tiled(rows, w_query, w_pool_in, w_out):
    counts = lax.axis_size("sp"), lax.axis_size("tp")
    return (
        all(count & (count - 1) == 0 for count in counts)
        and counts[0] >= 8
        and rows % (counts[1] * QB) == 0
        and rows % ROW_TILE == 0
        and w_query.shape[1] % LANES == 0
        and w_pool_in.shape[1] % LANES == 0
        and w_out.shape[1] % LANES == 0
        and counts[1] * w_query.shape[1] == QH * HEAD
    )


def body(*args):
    tokens, w_query, w_pool_in, w_out = args[0], args[2], args[5], args[8]
    if tiled(tokens.shape[0], w_query, w_pool_in, w_out):
        return fast_body(*args)
    return plain_body(*args)


def solution(mesh):
    in_specs = (
        P("sp", None),
        P(),
        P(None, "tp"),
        P("sp", None),
        P("sp", None),
        P(None, "tp"),
        P("tp"),
        P("tp"),
        P("tp", "sp"),
    )
    out_specs = P(("sp", "tp"), None)
    return jax.shard_map(body, mesh=mesh, in_specs=in_specs, out_specs=out_specs, check_vma=False)
```

```python
import functools

import jax
import jax.numpy as jnp
import numpy as np
from jax import lax
from jax.experimental import pallas as pl
from jax.experimental.pallas import tpu as pltpu
from jax.sharding import PartitionSpec as P

HEAD = 64
QH = 8
KVH = 2
POOL_CH = 128
WINDOW = 128
QB = 128


NEG_BIG = -1e30
POOL_SPANS = (2, 4, 8, 16)


def extended(block, sides, width):
    for axis, dim in sides:
        count = lax.axis_size(axis)
        forward = [(i, i + 1) for i in range(count - 1)]
        backward = [(target, source) for source, target in forward]
        low = lax.ppermute(
            lax.slice_in_dim(block, block.shape[dim] - width, None, axis=dim), axis, forward
        )
        high = lax.ppermute(lax.slice_in_dim(block, 0, width, axis=dim), axis, backward)
        block = jnp.concatenate([low, block, high], axis=dim)
    return block


def layer_normed(tokens, norm_gain):
    values = tokens.astype(jnp.float32)
    center = jnp.mean(values, axis=-1, keepdims=True)
    spread = jnp.mean(jnp.square(values - center), axis=-1, keepdims=True)
    return ((values - center) * lax.rsqrt(spread + 1e-06) * norm_gain).astype(jnp.bfloat16)


def rotate(values, positions):
    half = HEAD // 2
    inverse = 10000.0 ** (-jnp.arange(half, dtype=jnp.float32) / half)
    angles = positions[:, None] * inverse[None, :]
    cosine = jnp.cos(angles)[:, None, :]
    sine = jnp.sin(angles)[:, None, :]
    first = values[..., :half]
    second = values[..., half:]
    return jnp.concatenate(
        [first * cosine - second * sine, first * sine + second * cosine], axis=-1
    )


def plain_body(tokens, norm_gain, w_query, w_key, w_value, w_pool_in, sink_logit, pool_scale, w_out):
    local_rows = tokens.shape[0]
    seq_total = local_rows * lax.axis_size("sp")
    offset = lax.axis_index("sp") * local_rows
    tp_place = lax.axis_index("tp")
    local_heads = w_query.shape[1] // HEAD
    local_pool = w_pool_in.shape[1]
    reach = POOL_SPANS[-1] // 2
    normed = layer_normed(tokens, norm_gain)
    positions = (offset + jnp.arange(local_rows)).astype(jnp.float32)
    query = rotate(
        jnp.dot(normed, w_query, preferred_element_type=jnp.float32).reshape(
            local_rows, local_heads, HEAD
        ),
        positions,
    ).astype(jnp.bfloat16)
    key_head = tp_place * local_heads // (QH // KVH)
    key_cols = lax.dynamic_slice_in_dim(w_key, key_head * HEAD, HEAD, 1)
    value_cols = lax.dynamic_slice_in_dim(w_value, key_head * HEAD, HEAD, 1)
    key_sum = jnp.dot(
        normed,
        lax.all_gather(key_cols, "sp", axis=0, tiled=True),
        preferred_element_type=jnp.float32,
    )
    value_sum = jnp.dot(
        normed,
        lax.all_gather(value_cols, "sp", axis=0, tiled=True),
        preferred_element_type=jnp.float32,
    )
    key = rotate(key_sum[:, None, :], positions)[:, 0, :].astype(jnp.bfloat16)
    value = value_sum.astype(jnp.bfloat16)
    key_value = jnp.concatenate([key, value], axis=1)
    pool_in = jnp.dot(normed, w_pool_in, preferred_element_type=jnp.float32).astype(jnp.bfloat16)
    widened = extended(jnp.concatenate([key_value, pool_in], axis=1), (("sp", 0),), WINDOW)
    kv_wide = widened[:, : 2 * HEAD]
    pool_wide = widened[WINDOW - reach : WINDOW + local_rows + reach, 2 * HEAD :]
    span = QB + 2 * WINDOW
    sink_here = sink_logit[:, None, None]
    results = []
    for block in range(local_rows // QB):
        queries = query[block * QB : (block + 1) * QB]
        keys = kv_wide[block * QB : block * QB + span, :HEAD]
        values = kv_wide[block * QB : block * QB + span, HEAD:]
        scores = jnp.einsum(
            "ihd,jd->hij", queries, keys, preferred_element_type=jnp.float32
        ) * HEAD ** (-0.5)
        query_pos = offset + block * QB + jnp.arange(QB)
        key_pos = offset + block * QB - WINDOW + jnp.arange(span)
        valid = (
            (jnp.abs(query_pos[:, None] - key_pos[None, :]) <= WINDOW)
            & (key_pos[None, :] >= 0)
            & (key_pos[None, :] < seq_total)
        )
        scores = jnp.where(valid, scores, NEG_BIG)
        highest = jnp.maximum(jnp.max(scores, axis=-1, keepdims=True), sink_here)
        expo = jnp.where(valid, jnp.exp(scores - highest), 0.0)
        total = jnp.sum(expo, axis=-1, keepdims=True) + jnp.exp(sink_here - highest)
        weights = (expo / total).astype(jnp.bfloat16)
        result = jnp.einsum("hij,jd->ihd", weights, values, preferred_element_type=jnp.float32)
        results.append(result.reshape(QB, local_heads * HEAD).astype(jnp.bfloat16))
    attended = jnp.concatenate(results, axis=0)
    pool_vals = pool_wide.astype(jnp.float32)
    window_sum = pool_vals
    global_pos = offset + jnp.arange(local_rows)
    channel = tp_place * local_pool + jnp.arange(local_pool)
    window_group = channel // POOL_CH
    measured = jnp.zeros((local_rows, local_pool), jnp.float32)
    stride = 1
    for index, width in enumerate(POOL_SPANS):
        window_sum = window_sum[:-stride] + window_sum[stride:]
        stride = width
        sums = window_sum[reach - width // 2 : reach - width // 2 + local_rows]
        counted = (
            jnp.minimum(global_pos + width // 2, seq_total)
            - jnp.maximum(global_pos - width // 2, 0)
        ).astype(jnp.float32)
        measured = measured + jnp.where(
            window_group[None, :] == index, sums / counted[:, None], 0.0
        )
    pooled = ((measured - pool_vals[reach : reach + local_rows]) * pool_scale).astype(jnp.bfloat16)
    attended_rows, pooled_rows = (
        lax.all_to_all(attended, "tp", split_axis=0, concat_axis=1, tiled=True),
        lax.all_to_all(pooled, "tp", split_axis=0, concat_axis=1, tiled=True),
    )
    joined = jnp.concatenate([attended_rows, pooled_rows], axis=1)
    out_rows_all = lax.all_gather(w_out, "tp", axis=0, tiled=True)
    projected = jnp.dot(
        joined,
        lax.all_gather(out_rows_all, "sp", axis=1, tiled=True),
        preferred_element_type=jnp.float32,
    )
    return projected.astype(jnp.bfloat16)


LANES = 128
ROW_TILE = 256
BF16 = jnp.bfloat16
F32 = jnp.float32
INFO = 3
GRANT = 16 * 1024 * 1024


def whole():
    return pl.BlockSpec(memory_space=pltpu.VMEM)


def scalars():
    return pl.BlockSpec(memory_space=pltpu.SMEM)


def aligned(start, size=QB):
    return pl.ds(pl.multiple_of(start, QB), size)


def cost(flops, moved=0):
    return pl.CostEstimate(flops=flops, bytes_accessed=moved, transcendentals=0)


def rope_angles(block, base, blocks):
    (cosine, sine), row = (base[0], base[1]), pl.ds(block, 1)
    turn, lift = blocks[0, row, :], blocks[1, row, :]
    return cosine * turn - sine * lift, sine * turn + cosine * lift


def rope_lanes(values, angles):
    lane = lax.broadcasted_iota(jnp.int32, values.shape, 1)
    swapped = jnp.where(
        lane % HEAD < HEAD // 2,
        -pltpu.roll(values, LANES - HEAD // 2, 1),
        pltpu.roll(values, HEAD // 2, 1),
    )
    return values * angles[0] + swapped * angles[1]


def load_project_kernel(info, *refs):
    (tokens, *shared), (normed, query, pool), (rows, *kept) = refs[:6], refs[6:9], refs[9:15]
    sems = refs[15]
    size = normed.shape[0]
    tiles = tokens.shape[0] // size

    def tile(ref, index):
        return ref.at[index * size : (index + 1) * size, :]

    pairs = [(tile(tokens, 0), tile(rows, 0))] + list(zip(shared, kept))
    pairs += [(tile(tokens, index), tile(rows, index)) for index in range(1, tiles)]
    copies = [pltpu.make_async_copy(*pair, sems.at[index]) for index, pair in enumerate(pairs)]
    for copy in copies:
        copy.start()
    copies[0].wait()
    copies[1].wait()
    project_kernel(0, info, rows, *kept, normed, query, pool, ready=copies[2:6])
    for copy in copies[6:]:
        copy.wait()


def project_kernel(
    offset, info, tokens, gain, w_query, w_pool, base, blocks, normed, query, pool, ready=()
):
    size = normed.shape[0]
    for row in range(0, size, 16):
        values = tokens[offset + row : offset + row + 16, :].astype(F32)
        centred = values - jnp.mean(values, axis=-1, keepdims=True)
        spread = jnp.mean(centred * centred, axis=-1, keepdims=True)
        normed[row : row + 16, :] = (centred * lax.rsqrt(spread + 1e-06) * gain[...]).astype(BF16)
    for copy in ready:
        copy.wait()
    left = normed[...]
    pool[...] = jnp.dot(left, w_pool[...], preferred_element_type=F32).astype(BF16)
    products = jnp.dot(left, w_query[...], preferred_element_type=F32)
    first = info[0] * (tokens.shape[0] // QB) + offset // QB
    for row in range(0, size, QB):
        angles = rope_angles(first + row // QB, base, blocks)
        for lane in range(0, products.shape[1], LANES):
            turned = rope_lanes(products[row : row + QB, lane : lane + LANES], angles)
            query[row : row + QB, lane : lane + LANES] = turned.astype(BF16) * HEAD ** (-0.5)


def key_value_kernel(tiles, info, *refs):
    pieces, normed, pools = refs[:4], refs[4 : 4 + tiles], refs[4 + tiles : 6 + tiles]
    base, blocks, key_value, head, tail, weight = refs[6 + tiles :]
    depth = pieces[0].shape[1]
    for index, piece in enumerate(pieces):
        for slot in range(piece.shape[0]):
            place = info[INFO + index * piece.shape[0] + slot]
            weight[pl.ds(pl.multiple_of(place * depth, depth), depth), :] = piece[slot]
    size = normed[0].shape[0]
    first = info[0] * (key_value.shape[0] // QB)
    for tile in range(tiles):
        products = jnp.dot(normed[tile][...], weight[...], preferred_element_type=F32)
        lane = lax.broadcasted_iota(jnp.int32, (QB, LANES), 1)
        for row in range(0, size, QB):
            angles = rope_angles(first + (tile * size + row) // QB, base, blocks)
            plain = products[row : row + QB, :]
            result = jnp.where(lane < HEAD, rope_lanes(plain, angles), plain).astype(BF16)
            key_value[tile * size + row : tile * size + row + QB, :] = result
            if tile == 0 and row == 0:
                head[:WINDOW, :] = result
            if tile == tiles - 1 and row == size - QB:
                tail[:WINDOW, :] = result
    edge = (head.shape[0] - WINDOW) // (pools[0].shape[1] // LANES)
    for group in range(pools[0].shape[1] // LANES):
        lanes = slice(group * LANES, (group + 1) * LANES)
        rows = slice(WINDOW + group * edge, WINDOW + (group + 1) * edge)
        head[rows, :] = pools[0][:edge, lanes]
        tail[rows, :] = pools[1][size - edge :, lanes]


def pool_kernel(tiles, chunks, info, *refs):
    pools, (low, high, scale), outs = refs[:tiles], refs[tiles : tiles + 3], refs[tiles + 3 : -1]
    wide = refs[-1]
    size, channels = pools[0].shape
    rows = size * tiles
    edge = (wide.shape[0] - rows) // 2
    chunk = rows // chunks
    place, total = info[0], info[2] * rows
    tp = info[1]
    groups = channels // LANES
    for group in range(groups):
        start = WINDOW + group * edge
        lanes = slice(group * LANES, (group + 1) * LANES)
        wide[:edge, lanes] = low[start : start + edge, :]
        wide[edge + rows :, lanes] = high[start : start + edge, :]
    for tile in range(tiles):
        wide[edge + tile * size : edge + (tile + 1) * size, :] = pools[tile][...]
    span = QB + 2 * edge
    row = lax.broadcasted_iota(jnp.int32, (QB, span), 0) + edge
    column = lax.broadcasted_iota(jnp.int32, (QB, span), 1)
    bands, reaches = [], []
    for group in range(groups):
        reach = lax.shift_left(jnp.int32(1), tp * groups + group)
        inside = (column >= row - reach) & (column < row + reach)
        bands.append(jnp.where(inside, 1.0, 0.0).astype(BF16))
        reaches.append(reach)
    for step in range(chunks):
        target = lax.bitwise_xor(tp, step)
        for block in range(0, chunk, QB):
            start = target * chunk + block
            position = place * rows + start + lax.broadcasted_iota(jnp.int32, (QB, 1), 0)
            for group in range(groups):
                lanes = slice(group * LANES, (group + 1) * LANES)
                sums = jnp.dot(
                    bands[group],
                    wide[aligned(start, span), lanes],
                    preferred_element_type=F32,
                )
                counted = jnp.minimum(position + reaches[group], total) - jnp.maximum(
                    position - reaches[group], 0
                )
                mean = sums * (1.0 / counted.astype(F32))
                own = wide[pl.ds(pl.multiple_of(start + edge, edge), QB), lanes].astype(F32)
                outs[step][block : block + QB, lanes] = ((mean - own) * scale[:, lanes]).astype(BF16)


def attend_kernel(step, tiles, info, sink, *refs):
    pieces = refs[:tiles]
    key_value, low, high, out, keys, values, query = refs[tiles:]
    chunk = out.shape[0]
    size = pieces[0].shape[0]
    place, tp, count = info[0], info[1], info[2]
    target = lax.bitwise_xor(tp, step)
    total_rows = key_value.shape[0]
    chunks = total_rows // chunk
    for option in range(chunks):

        @pl.when(target == option)
        def _(option=option):
            for row in range(0, chunk, size):
                part = pieces[(option * chunk + row) // size]
                query[row : row + size, :] = part[...]

    begin = pl.multiple_of(target * chunk, chunk)

    def put(start, rows):
        wide = rows.astype(F32)
        lane = lax.broadcasted_iota(jnp.int32, wide.shape, 1)
        turned = pltpu.roll(wide, HEAD, 1)
        for side, (key, value) in enumerate(((wide, turned), (turned, wide))):
            first = lane < HEAD if side == 0 else lane >= HEAD
            keys[side, start : start + rows.shape[0], :] = jnp.where(first, key, 0.0).astype(BF16)
            values[side, start : start + rows.shape[0], :] = jnp.where(first, value, 0.0).astype(
                BF16
            )

    for block in range(0, chunk, QB):
        put(WINDOW + block, key_value[aligned(begin + block), :])
    before = key_value[aligned(jnp.maximum(begin - WINDOW, 0)), :]
    put(0, jnp.where(target == 0, low[:WINDOW, :], before))
    after_start = jnp.minimum(begin + chunk, total_rows - WINDOW)
    after = key_value[aligned(after_start), :]
    put(WINDOW + chunk, jnp.where(target == chunks - 1, high[:WINDOW, :], after))

    row = lax.broadcasted_iota(jnp.int32, (QB, WINDOW), 0)
    column = lax.broadcasted_iota(jnp.int32, (QB, WINDOW), 1)
    at_start = (place == 0) & (target == 0)
    at_end = (place == count - 1) & (target == chunks - 1)
    for block in range(0, chunk, QB):
        low_ok, high_ok = column >= row, column <= row
        if block == 0:
            low_ok = low_ok & jnp.logical_not(at_start)
        if block == chunk - QB:
            high_ok = high_ok & jnp.logical_not(at_end)
        for pair in range(query.shape[1] // LANES):
            lanes = slice(pair * LANES, (pair + 1) * LANES)
            queries = query[block : block + QB, lanes]
            result = None
            for side in range(2):
                scores = lax.dot_general(
                    queries,
                    keys[side, block : block + QB + 2 * WINDOW, :],
                    (((1,), (1,)), ((), ())),
                    preferred_element_type=F32,
                )
                parts = (
                    jnp.where(low_ok, scores[:, :WINDOW], NEG_BIG),
                    scores[:, WINDOW : WINDOW + QB],
                    jnp.where(high_ok, scores[:, WINDOW + QB :], NEG_BIG),
                )
                logit = sink[2 * pair + side]
                top = jnp.maximum(jnp.maximum(parts[0], parts[1]), parts[2])
                top = jnp.maximum(jnp.max(top, axis=-1, keepdims=True), logit)
                expo = [jnp.exp(part - top) for part in parts]
                total = jnp.sum(expo[0] + expo[1] + expo[2], axis=-1, keepdims=True)
                inverse = 1.0 / (total + jnp.exp(logit - top))
                weights = jnp.concatenate([(part * inverse).astype(BF16) for part in expo], axis=1)
                part = jnp.dot(
                    weights,
                    values[side, block : block + QB + 2 * WINDOW, :],
                    preferred_element_type=F32,
                )
                result = part if result is None else result + part
            out[block : block + QB, lanes] = result.astype(BF16)


def output_kernel(parts, offset, info, *refs):
    attended, pooled = refs[:parts], refs[parts : 2 * parts]
    sources, (out, joined, staged, out_sem) = refs[2 * parts : 2 * parts + 4], refs[2 * parts + 4 :]
    order = (0, 2, 1, 3)
    tp = info[1]
    width = attended[0].shape[1]
    for step in range(parts):
        owner = lax.bitwise_xor(tp, step)
        for half, part in enumerate((attended[step], pooled[step])):
            start = pl.multiple_of((half * parts + owner) * width, LANES)
            joined[:, pl.ds(start, width)] = part[...]
    depth, lanes = sources[0].shape[1], sources[0].shape[2]
    blocks = sources[0].shape[0] // parts
    stores = []
    for index in order:
        for block in range(0, blocks, 2):
            total = None
            entries = [(index * blocks + block + side) * (parts + 1) for side in range(2)]
            for step in range(parts):
                start = pl.multiple_of(lax.bitwise_xor(tp, step) * depth, LANES)
                right = jnp.concatenate(
                    [sources[index][info[offset + entry + 1 + step]] for entry in entries], axis=1
                )
                product = jnp.dot(
                    joined[:, pl.ds(start, depth)], right, preferred_element_type=F32
                )
                total = product if total is None else total + product
            for side in range(2):
                number = index * blocks + block + side
                staged[number] = total[:, side * lanes : (side + 1) * lanes].astype(BF16)
                start = pl.multiple_of(info[offset + entries[side]] * lanes, LANES)
                store = pltpu.make_async_copy(
                    staged.at[number], out.at[:, pl.ds(start, lanes)], out_sem.at[number]
                )
                store.start()
                stores.append(store)
    for store in stores:
        store.wait()


def exchange_orders(sp_count, tp_count):
    sp_bits = [tp_count << bit for bit in range(1, sp_count.bit_length() - 1)][::-1]
    tp_bits = [1 << bit for bit in range(tp_count.bit_length() - 1)]
    for bits in (sp_bits, sp_bits[:1] + tp_bits + sp_bits[1:]):
        yield bits, bits[-1:] + bits[:-1]


def slot_masks(bits):
    masks = [0]
    for bit in bits:
        masks = masks + [mask ^ bit for mask in masks]
    return masks


def doubled(block, orders, sp_count, tp_count):
    even, odd = orders
    devices = range(sp_count * tp_count)

    def send(array, masks):
        pairs = [(i, i ^ masks[(i // tp_count) & 1]) for i in devices]
        return lax.ppermute(array, ("sp", "tp"), pairs)

    held = block[None]
    for masks in zip(even[:-1], odd[:-1]):
        held = jnp.concatenate([held, send(held, masks)], axis=0)
    core = (tp_count, tp_count)
    came = send(held, (even[-1], odd[-1]))
    return held, came, send(held, core), send(came, core)


def device_table(sp_count, tp_count, kv_orders, out_orders):
    rows = []
    for sp_place in range(sp_count):
        for tp_place in range(tp_count):
            kinds = [sp_place % 2, 1 - sp_place % 2]
            kv_part, out_part = [], []
            for flip, kind in enumerate(kinds):
                for late in range(2):
                    order = kv_orders[kind]
                    extra = order[-1] * late
                    for mask in slot_masks(order[:-1]):
                        kv_part.append(sp_place ^ flip ^ ((mask ^ extra) // tp_count))
                    order = out_orders[kind]
                    extra = order[-1] * late
                    found = {}
                    for slot, mask in enumerate(slot_masks(order[:-1])):
                        delta, step = divmod(mask ^ extra, tp_count)
                        found.setdefault(delta, {})[step] = slot
                    for delta, slots in found.items():
                        out_part.append(sp_place ^ flip ^ delta)
                        out_part += [slots[step] for step in range(tp_count)]
            rows.append([sp_place, tp_place, sp_count] + kv_part + out_part)
    return np.array(rows, np.int32)


def rope_tables(length):
    half = HEAD // 2
    inverse = np.float32(10000.0) ** (-np.arange(half, dtype=np.float32) / np.float32(half))
    inverse = np.tile(inverse.astype(np.float64), LANES // half)
    tables = []
    for positions in (np.arange(QB), np.arange(0, length, QB)):
        angles = positions[:, None] * inverse[None, :]
        tables.append(np.stack([np.cos(angles), np.sin(angles)]).astype(np.float32))
    return tables


def fast_body(tokens, norm_gain, w_query, w_key, w_value, w_pool_in, sink_logit, pool_scale, w_out):
    sp_count, tp_count = lax.axis_size("sp"), lax.axis_size("tp")
    local_rows, width = tokens.shape
    sp_place, tp_place = lax.axis_index("sp"), lax.axis_index("tp")
    local_heads = w_query.shape[1] // HEAD
    heads_width, local_pool = w_query.shape[1], w_pool_in.shape[1]
    chunk = local_rows // tp_count
    kv_orders, out_orders = exchange_orders(sp_count, tp_count)

    key_head = tp_place * local_heads // (QH // KVH)
    kv_block = jnp.concatenate(
        [lax.dynamic_slice_in_dim(w, key_head * HEAD, HEAD, 1) for w in (w_key, w_value)], axis=1
    )
    kv_pieces = doubled(kv_block, kv_orders, sp_count, tp_count)
    out_pieces = doubled(w_out, out_orders, sp_count, tp_count)

    table = device_table(sp_count, tp_count, kv_orders, out_orders)
    info = lax.dynamic_index_in_dim(jnp.array(table), sp_place * tp_count + tp_place, 0, False)
    base, blocks = (jnp.array(t) for t in rope_tables(local_rows * sp_count))

    def call(name, kernel, operands, specs, out_shape, scratch, flops):
        single = not isinstance(out_shape, list)
        shapes = [
            jax.ShapeDtypeStruct(*(shape if isinstance(shape[0], tuple) else (shape, BF16)))
            for shape in ([out_shape] if single else out_shape)
        ]
        spec = pltpu.HBM if name == "output" else pltpu.VMEM
        outs = [pl.BlockSpec(memory_space=spec)] * len(shapes)
        return pl.pallas_call(
            kernel,
            in_specs=specs,
            out_specs=outs[0] if single else outs,
            out_shape=shapes[0] if single else shapes,
            scratch_shapes=scratch,
            compiler_params=pltpu.CompilerParams(vmem_limit_bytes=GRANT),
            cost_estimate=cost(flops),
        )(*operands)

    tiles = local_rows // ROW_TILE
    normed, queries, pools = [], [], []
    results = [(ROW_TILE, width), (ROW_TILE, heads_width), (ROW_TILE, local_pool)]
    held = (tokens, norm_gain[None, :], w_query, w_pool_in, base, blocks)
    held = tuple(pltpu.with_memory_space_constraint(part, pltpu.HBM) for part in held)
    for tile in range(tiles):
        flops = 2 * ROW_TILE * width * (heads_width + local_pool)
        if tile == 0:
            outs = call(
                "project0",
                load_project_kernel,
                (info, *held),
                [scalars()] + [pl.BlockSpec(memory_space=pltpu.HBM)] * 6,
                results + [(part.shape, part.dtype) for part in held],
                [pltpu.SemaphoreType.DMA((5 + tiles,))],
                flops,
            )
            held = outs[3:]
        else:
            outs = call(
                f"project{tile}",
                functools.partial(project_kernel, tile * ROW_TILE),
                (info, *held),
                [scalars()] + [whole()] * 6,
                results,
                [],
                flops,
            )
        for found, out in zip((normed, queries, pools), outs):
            found.append(out)

    edge = 2 * (POOL_SPANS[-1] // 2)
    payload = (WINDOW + edge * (local_pool // LANES), LANES)
    key_value, head, tail = call(
        "key_value",
        functools.partial(key_value_kernel, tiles),
        (info, *kv_pieces, *normed, pools[0], pools[-1], *held[4:]),
        [scalars()] + [whole()] * (8 + tiles),
        [(local_rows, LANES), payload, payload],
        [pltpu.VMEM((width, LANES), BF16)],
        2 * local_rows * width * LANES,
    )

    forward = [(i, i + 1) for i in range(sp_count - 1)]
    low = lax.ppermute(tail, "sp", forward)
    high = lax.ppermute(head, "sp", [(target, source) for source, target in forward])

    devices = range(tp_count)
    pooled = call(
        "pool",
        functools.partial(pool_kernel, tiles, tp_count),
        (info, *pools, low, high, pool_scale[None, :]),
        [scalars()] + [whole()] * (tiles + 3),
        [(chunk, local_pool)] * tp_count,
        [pltpu.VMEM((local_rows + 2 * edge, local_pool), BF16)],
        2 * local_rows * local_pool * 160,
    )

    def hand_over(part, step):
        if step == 0:
            return part
        return lax.ppermute(part, "tp", [(i, i ^ step) for i in devices])

    pooled_parts = [hand_over(pooled[step], step) for step in devices]

    attended_parts = [None] * tp_count
    for step in list(devices)[1:] + [0]:
        attended = call(
            f"attend{step}",
            functools.partial(attend_kernel, step, tiles),
            (info, sink_logit, *queries, key_value, low, high),
            [scalars(), scalars()] + [whole()] * (tiles + 3),
            (chunk, heads_width),
            [pltpu.VMEM((2, chunk + 2 * WINDOW, LANES), BF16)] * 2
            + [pltpu.VMEM((chunk, heads_width), BF16)],
            4 * chunk * 3 * WINDOW * LANES * local_heads,
        )
        attended_parts[step] = hand_over(attended, step)

    columns = w_out.shape[1] * sp_count
    return call(
        "output",
        functools.partial(output_kernel, tp_count, INFO + sp_count),
        (info, *attended_parts, *pooled_parts, *out_pieces),
        [scalars()] + [whole()] * (2 * tp_count) + [whole()] * 4,
        (chunk, columns),
        [
            pltpu.VMEM((chunk, w_out.shape[0] * tp_count), BF16),
            pltpu.VMEM((sp_count, chunk, w_out.shape[1]), BF16),
            pltpu.SemaphoreType.DMA((sp_count,)),
        ],
        2 * chunk * columns * w_out.shape[0] * tp_count,
    )


def tiled(rows, w_query, w_pool_in, w_out):
    counts = lax.axis_size("sp"), lax.axis_size("tp")
    return (
        all(count & (count - 1) == 0 for count in counts)
        and counts[0] >= 8
        and rows % (counts[1] * QB) == 0
        and rows % ROW_TILE == 0
        and w_query.shape[1] % LANES == 0
        and w_pool_in.shape[1] % LANES == 0
        and w_out.shape[1] % LANES == 0
        and counts[1] * w_query.shape[1] == QH * HEAD
    )


def body(*args):
    tokens, w_query, w_pool_in, w_out = args[0], args[2], args[5], args[8]
    if tiled(tokens.shape[0], w_query, w_pool_in, w_out):
        return fast_body(*args)
    return plain_body(*args)


def solution(mesh):
    in_specs = (
        P("sp", None),
        P(),
        P(None, "tp"),
        P("sp", None),
        P("sp", None),
        P(None, "tp"),
        P("tp"),
        P("tp"),
        P("tp", "sp"),
    )
    out_specs = P(("sp", "tp"), None)
    return jax.shard_map(body, mesh=mesh, in_specs=in_specs, out_specs=out_specs, check_vma=False)
```

```python
import functools

import jax
import jax.numpy as jnp
import numpy as np
from jax import lax
from jax.experimental import pallas as pl
from jax.experimental.pallas import tpu as pltpu
from jax.sharding import PartitionSpec as P

HEAD = 64
QH = 8
KVH = 2
POOL_CH = 128
WINDOW = 128
QB = 128


NEG_BIG = -1e30
POOL_SPANS = (2, 4, 8, 16)


def extended(block, sides, width):
    for axis, dim in sides:
        count = lax.axis_size(axis)
        forward = [(i, i + 1) for i in range(count - 1)]
        backward = [(target, source) for source, target in forward]
        low = lax.ppermute(
            lax.slice_in_dim(block, block.shape[dim] - width, None, axis=dim), axis, forward
        )
        high = lax.ppermute(lax.slice_in_dim(block, 0, width, axis=dim), axis, backward)
        block = jnp.concatenate([low, block, high], axis=dim)
    return block


def layer_normed(tokens, norm_gain):
    values = tokens.astype(jnp.float32)
    center = jnp.mean(values, axis=-1, keepdims=True)
    spread = jnp.mean(jnp.square(values - center), axis=-1, keepdims=True)
    return ((values - center) * lax.rsqrt(spread + 1e-06) * norm_gain).astype(jnp.bfloat16)


def rotate(values, positions):
    half = HEAD // 2
    inverse = 10000.0 ** (-jnp.arange(half, dtype=jnp.float32) / half)
    angles = positions[:, None] * inverse[None, :]
    cosine = jnp.cos(angles)[:, None, :]
    sine = jnp.sin(angles)[:, None, :]
    first = values[..., :half]
    second = values[..., half:]
    return jnp.concatenate(
        [first * cosine - second * sine, first * sine + second * cosine], axis=-1
    )


def plain_body(tokens, norm_gain, w_query, w_key, w_value, w_pool_in, sink_logit, pool_scale, w_out):
    local_rows = tokens.shape[0]
    seq_total = local_rows * lax.axis_size("sp")
    offset = lax.axis_index("sp") * local_rows
    tp_place = lax.axis_index("tp")
    local_heads = w_query.shape[1] // HEAD
    local_pool = w_pool_in.shape[1]
    reach = POOL_SPANS[-1] // 2
    normed = layer_normed(tokens, norm_gain)
    positions = (offset + jnp.arange(local_rows)).astype(jnp.float32)
    query = rotate(
        jnp.dot(normed, w_query, preferred_element_type=jnp.float32).reshape(
            local_rows, local_heads, HEAD
        ),
        positions,
    ).astype(jnp.bfloat16)
    key_head = tp_place * local_heads // (QH // KVH)
    key_cols = lax.dynamic_slice_in_dim(w_key, key_head * HEAD, HEAD, 1)
    value_cols = lax.dynamic_slice_in_dim(w_value, key_head * HEAD, HEAD, 1)
    key_sum = jnp.dot(
        normed,
        lax.all_gather(key_cols, "sp", axis=0, tiled=True),
        preferred_element_type=jnp.float32,
    )
    value_sum = jnp.dot(
        normed,
        lax.all_gather(value_cols, "sp", axis=0, tiled=True),
        preferred_element_type=jnp.float32,
    )
    key = rotate(key_sum[:, None, :], positions)[:, 0, :].astype(jnp.bfloat16)
    value = value_sum.astype(jnp.bfloat16)
    key_value = jnp.concatenate([key, value], axis=1)
    pool_in = jnp.dot(normed, w_pool_in, preferred_element_type=jnp.float32).astype(jnp.bfloat16)
    widened = extended(jnp.concatenate([key_value, pool_in], axis=1), (("sp", 0),), WINDOW)
    kv_wide = widened[:, : 2 * HEAD]
    pool_wide = widened[WINDOW - reach : WINDOW + local_rows + reach, 2 * HEAD :]
    span = QB + 2 * WINDOW
    sink_here = sink_logit[:, None, None]
    results = []
    for block in range(local_rows // QB):
        queries = query[block * QB : (block + 1) * QB]
        keys = kv_wide[block * QB : block * QB + span, :HEAD]
        values = kv_wide[block * QB : block * QB + span, HEAD:]
        scores = jnp.einsum(
            "ihd,jd->hij", queries, keys, preferred_element_type=jnp.float32
        ) * HEAD ** (-0.5)
        query_pos = offset + block * QB + jnp.arange(QB)
        key_pos = offset + block * QB - WINDOW + jnp.arange(span)
        valid = (
            (jnp.abs(query_pos[:, None] - key_pos[None, :]) <= WINDOW)
            & (key_pos[None, :] >= 0)
            & (key_pos[None, :] < seq_total)
        )
        scores = jnp.where(valid, scores, NEG_BIG)
        highest = jnp.maximum(jnp.max(scores, axis=-1, keepdims=True), sink_here)
        expo = jnp.where(valid, jnp.exp(scores - highest), 0.0)
        total = jnp.sum(expo, axis=-1, keepdims=True) + jnp.exp(sink_here - highest)
        weights = (expo / total).astype(jnp.bfloat16)
        result = jnp.einsum("hij,jd->ihd", weights, values, preferred_element_type=jnp.float32)
        results.append(result.reshape(QB, local_heads * HEAD).astype(jnp.bfloat16))
    attended = jnp.concatenate(results, axis=0)
    pool_vals = pool_wide.astype(jnp.float32)
    window_sum = pool_vals
    global_pos = offset + jnp.arange(local_rows)
    channel = tp_place * local_pool + jnp.arange(local_pool)
    window_group = channel // POOL_CH
    measured = jnp.zeros((local_rows, local_pool), jnp.float32)
    stride = 1
    for index, width in enumerate(POOL_SPANS):
        window_sum = window_sum[:-stride] + window_sum[stride:]
        stride = width
        sums = window_sum[reach - width // 2 : reach - width // 2 + local_rows]
        counted = (
            jnp.minimum(global_pos + width // 2, seq_total)
            - jnp.maximum(global_pos - width // 2, 0)
        ).astype(jnp.float32)
        measured = measured + jnp.where(
            window_group[None, :] == index, sums / counted[:, None], 0.0
        )
    pooled = ((measured - pool_vals[reach : reach + local_rows]) * pool_scale).astype(jnp.bfloat16)
    attended_rows, pooled_rows = (
        lax.all_to_all(attended, "tp", split_axis=0, concat_axis=1, tiled=True),
        lax.all_to_all(pooled, "tp", split_axis=0, concat_axis=1, tiled=True),
    )
    joined = jnp.concatenate([attended_rows, pooled_rows], axis=1)
    out_rows_all = lax.all_gather(w_out, "tp", axis=0, tiled=True)
    projected = jnp.dot(
        joined,
        lax.all_gather(out_rows_all, "sp", axis=1, tiled=True),
        preferred_element_type=jnp.float32,
    )
    return projected.astype(jnp.bfloat16)


LANES = 128
ROW_TILE = 256
GRANT = 16 * 1024 * 1024
BF16 = jnp.bfloat16
F32 = jnp.float32


def whole():
    return pl.BlockSpec(memory_space=pltpu.VMEM)


def aligned(start, size=QB, multiple=QB):
    return pl.ds(pl.multiple_of(start, multiple), size)


def here():
    return lax.axis_index("sp"), lax.axis_index("tp")


def rope_angles(block, base, blocks):
    (cosine, sine), row = (base[0], base[1]), pl.ds(block, 1)
    turn, lift = blocks[0, row, :], blocks[1, row, :]
    return cosine * turn - sine * lift, sine * turn + cosine * lift


def rope_lanes(values, angles):
    lane = lax.broadcasted_iota(jnp.int32, values.shape, 1)
    swapped = jnp.where(
        lane % HEAD < HEAD // 2,
        -pltpu.roll(values, LANES - HEAD // 2, 1),
        pltpu.roll(values, HEAD // 2, 1),
    )
    return values * angles[0] + swapped * angles[1]


def norm_kernel(*refs):
    (tokens, gain, *shared), (normed, *kept), (rows, scale, sems) = refs[:6], refs[6:11], refs[11:]
    tiles = tokens.shape[0] // ROW_TILE

    def tile(ref, index):
        return ref.at[index * ROW_TILE : (index + 1) * ROW_TILE, :]

    pairs = [(gain, scale)] + [(tile(tokens, index), tile(rows, index)) for index in range(tiles)]
    pairs += list(zip(shared, kept))
    copies = [pltpu.make_async_copy(*pair, sems.at[index]) for index, pair in enumerate(pairs)]
    for copy in copies:
        copy.start()
    copies[0].wait()
    for index in range(tiles):
        copies[1 + index].wait()

        for row in range(index * ROW_TILE, (index + 1) * ROW_TILE, 16):
            place = slice(row, row + 16)
            values = rows[place, :].astype(F32)
            centred = values - jnp.mean(values, axis=-1, keepdims=True)
            spread = jnp.mean(centred * centred, axis=-1, keepdims=True)
            normed[place, :] = (centred * lax.rsqrt(spread + 1e-06) * scale[...]).astype(BF16)

    for copy in copies[1 + tiles :]:
        copy.wait()


def band(group, groups, edge):
    row = lax.broadcasted_iota(jnp.int32, (QB, QB + 2 * edge), 0) + edge
    column = lax.broadcasted_iota(jnp.int32, (QB, QB + 2 * edge), 1)
    reach = lax.shift_left(jnp.int32(1), here()[1] * groups + group)
    inside = (column >= row - reach) & (column < row + reach)
    return reach, jnp.where(inside, 1.0, 0.0).astype(BF16)


def inner_blocks(blocks):
    half = blocks // 2
    tp = here()[1]
    return half - 1, (jnp.where(tp == 1, 1, half), jnp.where(tp == 0, 1, half))


def pool_kernel(edge, normed, w_pool, scale, pool, *outs):
    rows, channels = pool.shape
    weight = w_pool[...]

    @pl.loop(0, rows // ROW_TILE)
    def _(tile):
        place = aligned(tile * ROW_TILE, ROW_TILE)
        pool[place, :] = jnp.dot(normed[place, :], weight, preferred_element_type=F32).astype(BF16)

    groups = channels // LANES
    bands = [band(group, groups, edge) for group in range(groups)]
    count, firsts = inner_blocks(rows // QB)
    for first, out in zip(firsts, outs):

        @pl.loop(0, count)
        def _(step, first=first, out=out):
            start = (first + step) * QB
            for group, (reach, inside) in enumerate(bands):
                lanes = slice(group * LANES, (group + 1) * LANES)
                wide = pool[aligned(start - edge, QB + 2 * edge, edge), lanes]
                sums = jnp.dot(inside, wide, preferred_element_type=F32)
                own = pool[aligned(start), lanes].astype(F32)
                mean = sums * (0.5 / lax.convert_element_type(reach, F32))
                out[aligned(step * QB), lanes] = ((mean - own) * scale[:, lanes]).astype(BF16)


def query_kernel(normed, w_query, base, blocks, query):
    weight = w_query[...]
    first = here()[0] * (query.shape[0] // QB)

    @pl.loop(0, query.shape[0] // ROW_TILE)
    def _(tile):
        products = jnp.dot(
            normed[aligned(tile * ROW_TILE, ROW_TILE), :], weight, preferred_element_type=F32
        )
        for row in range(0, ROW_TILE, QB):
            angles = rope_angles(first + tile * (ROW_TILE // QB) + row // QB, base, blocks)
            for lane in range(0, query.shape[1], LANES):
                turned = rope_lanes(products[row : row + QB, lane : lane + LANES], angles)
                query[aligned(tile * ROW_TILE + row), lane : lane + LANES] = (
                    turned.astype(BF16) * HEAD ** (-0.5)
                )


def key_value_kernel(orders, sp_step, *refs):
    pieces, (normed, pool, base, blocks) = refs[:2], refs[2:6]
    key_value, first_out, second_out, weight = refs[6:]
    sp = here()[0]
    odd = sp % 2
    depth = pieces[0].shape[1]
    for flip, piece in enumerate(pieces):
        for slot, masks in enumerate(zip(*(slot_masks(order) for order in orders))):
            even_mask, odd_mask = (mask // sp_step for mask in masks)
            picked = jnp.where(odd == flip, even_mask, odd_mask)
            place = lax.bitwise_xor(sp, lax.bitwise_xor(picked, flip))
            weight[aligned(place * depth, depth), :] = piece[slot]
    right = weight[...]
    rows = key_value.shape[0]

    @pl.loop(0, rows // ROW_TILE)
    def _(tile):
        place = aligned(tile * ROW_TILE, ROW_TILE)
        products = jnp.dot(normed[place, :], right, preferred_element_type=F32)
        lane = lax.broadcasted_iota(jnp.int32, (QB, LANES), 1)
        for row in range(0, ROW_TILE, QB):
            block = tile * (ROW_TILE // QB) + row // QB
            angles = rope_angles(sp * (rows // QB) + block, base, blocks)
            plain = products[row : row + QB, :]
            result = jnp.where(lane < HEAD, rope_lanes(plain, angles), plain).astype(BF16)
            key_value[aligned(block * QB), :] = result

    groups = pool.shape[1] // LANES
    edge = (first_out.shape[0] - WINDOW) // groups
    for parity, (head, tail) in enumerate(((second_out, first_out), (first_out, second_out))):

        @pl.when(odd == parity)
        def _(head=head, tail=tail):
            head[:WINDOW, :] = key_value[:WINDOW, :]
            tail[:WINDOW, :] = key_value[rows - WINDOW :, :]
            for group in range(groups):
                lanes = slice(group * LANES, (group + 1) * LANES)
                place = slice(WINDOW + group * edge, WINDOW + (group + 1) * edge)
                head[place, :] = pool[:edge, lanes]
                tail[place, :] = pool[rows - edge :, lanes]


def split_halves(rows):
    wide = rows.astype(F32)
    first = lax.broadcasted_iota(jnp.int32, wide.shape, 1) < HEAD
    turned = pltpu.roll(wide, HEAD, 1)
    return jnp.where(first, wide, turned).astype(BF16), jnp.where(first, turned, wide).astype(BF16)


def attend_block(queries, keys, values, low_ok, high_ok, sink):
    first = lax.broadcasted_iota(jnp.int32, (QB, LANES), 1) < HEAD
    zero = jnp.zeros((QB, LANES), BF16)
    split = []
    for start in range(0, queries.shape[1], LANES):
        pair = queries[:, start : start + LANES]
        split += [jnp.where(first, pair, zero), jnp.where(first, zero, pair)]
    scores = lax.dot_general(
        jnp.concatenate(split, axis=0),
        keys,
        (((1,), (1,)), ((), ())),
        preferred_element_type=F32,
    )
    masked, weights = [], []
    for head in range(len(split)):
        part = scores[head * QB : (head + 1) * QB, :]
        parts = (
            jnp.where(low_ok, part[:, :WINDOW], NEG_BIG),
            part[:, WINDOW : WINDOW + QB],
            jnp.where(high_ok, part[:, WINDOW + QB :], NEG_BIG),
        )
        top = jnp.maximum(jnp.maximum(parts[0], parts[1]), parts[2])
        masked.append((parts, jnp.maximum(jnp.max(top, axis=-1, keepdims=True), sink[head])))
    for head, (parts, top) in enumerate(masked):
        expo = [jnp.exp(part - top) for part in parts]
        total = jnp.sum(expo[0] + expo[1] + expo[2], axis=-1, keepdims=True)
        inverse = 1.0 / (total + jnp.exp(sink[head] - top))
        weights.append(jnp.concatenate([(part * inverse).astype(BF16) for part in expo], axis=1))
    result = jnp.dot(jnp.concatenate(weights, axis=0), values, preferred_element_type=F32)
    heads = [result[head * QB : (head + 1) * QB, :] for head in range(len(split))]
    pairs = [jnp.where(first, *pair).astype(BF16) for pair in zip(heads[::2], heads[1::2])]
    return jnp.concatenate(pairs, axis=1)


def inside_window():
    row = lax.broadcasted_iota(jnp.int32, (QB, WINDOW), 0)
    column = lax.broadcasted_iota(jnp.int32, (QB, WINDOW), 1)
    return column >= row, column <= row


def inner_kernel(sink, query, key_value, given, kept, keys, values):
    blocks = query.shape[0] // QB

    @pl.loop(0, blocks)
    def _(block):
        place = aligned(block * QB)
        keys[place, :], values[place, :] = split_halves(key_value[place, :])

    low_ok, high_ok = inside_window()
    count, firsts = inner_blocks(blocks)

    @pl.loop(0, count)
    def _(step):
        for first, out in zip(firsts, (given, kept)):
            block = first + step
            span = aligned((block - 1) * QB, QB + 2 * WINDOW)
            out[aligned(step * QB), :] = attend_block(
                query[aligned(block * QB), :], keys[span, :], values[span, :], low_ok, high_ok, sink
            )


def outer_kernel(sp_count, sink, query, key_value, pool, scale, first, second, *outs):
    sp, tp = here()
    even = sp % 2 == 0
    rows, channels = pool.shape
    heads_width = query.shape[1]
    last = rows // QB - 1
    groups = channels // LANES
    edge = (first.shape[0] - WINDOW) // groups
    low_inside, high_inside = inside_window()
    bands = [band(group, groups, edge) for group in range(groups)]
    for step, out in enumerate(outs):
        at_front = lax.bitwise_xor(tp, step) == 1
        block = jnp.where(at_front, 0, last)
        coming = jnp.where(even == at_front, second[...], first[...])
        ahead, behind = key_value[: 2 * QB, :], key_value[rows - 2 * QB :, :]
        thirds = (
            jnp.where(at_front, coming[:WINDOW, :], behind[:QB, :]),
            jnp.where(at_front, ahead[:QB, :], behind[QB:, :]),
            jnp.where(at_front, ahead[QB:, :], coming[:WINDOW, :]),
        )
        keys, values = split_halves(jnp.concatenate(thirds, axis=0))
        low_ok = low_inside & jnp.logical_not(at_front & (sp == 0))
        high_ok = high_inside & (at_front | (sp != sp_count - 1))
        out[:, :heads_width] = attend_block(
            query[aligned(block * QB), :], keys, values, low_ok, high_ok, sink
        )
        position = sp * rows + block * QB + lax.broadcasted_iota(jnp.int32, (QB, 1), 0)
        for group, (reach, inside) in enumerate(bands):
            lanes = slice(group * LANES, (group + 1) * LANES)
            place = slice(WINDOW + group * edge, WINDOW + (group + 1) * edge)
            near, far = pool[: QB + edge, lanes], pool[rows - QB - edge :, lanes]
            front = jnp.concatenate([coming[place, :], near], axis=0)
            back = jnp.concatenate([far, coming[place, :]], axis=0)
            sums = jnp.dot(inside, jnp.where(at_front, front, back), preferred_element_type=F32)
            counted = jnp.minimum(position + reach, sp_count * rows) - jnp.maximum(
                position - reach, 0
            )
            mean = sums * (1.0 / counted.astype(F32))
            own = pool[aligned(block * QB), lanes].astype(F32)
            start = heads_width + group * LANES
            out[:, start : start + LANES] = ((mean - own) * scale[:, lanes]).astype(BF16)


def join_kernel(*refs):
    parts, joined = refs[:6], refs[6]
    tp = here()[1]
    inner, width = parts[0].shape
    count = joined.shape[0] - inner
    inner_rows = aligned((1 - tp) * count, inner)
    edge_rows = aligned(tp * inner, count)
    for side, (attended, pooled, edges) in enumerate((parts[:3], parts[3:])):
        owner = lax.bitwise_xor(tp, side)
        for half, part in enumerate((attended, pooled)):
            columns = pl.ds(pl.multiple_of((half * 2 + owner) * width, LANES), width)
            joined[inner_rows, columns] = part[...]
            joined[edge_rows, columns] = edges[:, half * width : (half + 1) * width]


def output_kernel(pieces, joined_parts, *refs):
    count = len(pieces)
    sources, refs = refs[:count], refs[count:]
    if joined_parts:
        parts, (out, joined, staged, sems) = refs[:6], refs[6:]
        join_kernel(*parts, joined)
    else:
        joined, _, out, staged, sems = refs
    sp, tp = here()
    depth, lanes = sources[0].shape[1], sources[0].shape[2]
    pairs = sources[0].shape[0] // 4
    stores = []

    def store(number, column):
        start = pl.multiple_of(column * lanes, LANES)
        return pltpu.make_async_copy(
            staged.at[number], out.at[:, pl.ds(start, lanes)], sems.at[number]
        )

    for index, (source, (flip, tables)) in enumerate(zip(sources, pieces)):
        kind = lax.bitwise_xor(sp % 2, flip)

        def entry(column, field, tables=tables, kind=kind):
            picked = jnp.int32(0)
            for place, values in enumerate(zip(*tables)):
                value = jnp.where(kind == 0, values[0][field], values[1][field])
                picked = jnp.where(column == place, value, picked)
            return picked

        @pl.loop(0, pairs)
        def _(pair, index=index, source=source, entry=entry, flip=flip):
            total = None
            for side in range(2):
                start = pl.multiple_of(lax.bitwise_xor(tp, side) * depth, LANES)
                right = jnp.concatenate(
                    [source[entry(2 * pair + half, 1 + side)] for half in range(2)], axis=1
                )
                product = jnp.dot(
                    joined[:, pl.ds(start, depth)], right, preferred_element_type=F32
                )
                total = product if total is None else total + product
            for half in range(2):
                number = index * 2 * pairs + 2 * pair + half
                staged[number] = total[:, half * lanes : (half + 1) * lanes].astype(BF16)
                delta = lax.bitwise_xor(entry(2 * pair + half, 0), flip)
                store(number, lax.bitwise_xor(sp, delta)).start()

        stores += [index * 2 * pairs + number for number in range(2 * pairs)]
    for number in stores:
        store(number, 0).wait()


def exchange_orders(sp_count, tp_count):
    sp_bits = [tp_count << bit for bit in range(1, sp_count.bit_length() - 1)][::-1]
    tp_bits = [1 << bit for bit in range(tp_count.bit_length() - 1)]
    mixed = sp_bits[:1] + tp_bits + sp_bits[1:]
    return (sp_bits[-1:] + sp_bits[:-1], sp_bits), (mixed, mixed[-1:] + mixed[:-1])


def slot_masks(bits):
    masks = [0]
    for bit in bits:
        masks = masks + [mask ^ bit for mask in masks]
    return masks


def output_tables(orders, late, tp_count):
    tables = []
    for order in orders:
        found = {}
        for slot, mask in enumerate(slot_masks(order[:-1])):
            delta, step = divmod(mask ^ (order[-1] * late), tp_count)
            found.setdefault(delta, {})[step] = slot
        tables.append([[delta, *(slots[t] for t in range(tp_count))] for delta, slots in found.items()])
    return tables


def doubled(block, orders, sp_count, tp_count, together):
    even, odd = orders
    devices = range(sp_count * tp_count)

    def send(array, masks):
        pairs = [(i, i ^ masks[(i // tp_count) & 1]) for i in devices]
        return lax.ppermute(array, ("sp", "tp"), pairs)

    held = block[None]
    for masks in zip(even[:-1], odd[:-1]):
        held = jnp.concatenate([held, send(held, masks)], axis=0)
    core = (tp_count, tp_count)
    came = send(held, (even[-1], odd[-1]))
    if together:
        held = jnp.concatenate([held, came], axis=0)
        return held, send(held, core)
    return held, came, send(held, core), send(came, core)


def rope_tables(length):
    half = HEAD // 2
    inverse = np.float32(10000.0) ** (-np.arange(half, dtype=np.float32) / np.float32(half))
    inverse = np.tile(inverse.astype(np.float64), LANES // half)
    tables = []
    for positions in (np.arange(QB), np.arange(0, length, QB)):
        angles = positions[:, None] * inverse[None, :]
        tables.append(np.stack([np.cos(angles), np.sin(angles)]).astype(np.float32))
    return tables


def call(kernel, operands, outs, scratch, flops, scalar=0, space=pltpu.VMEM, **more):
    specs = [pl.BlockSpec(memory_space=pltpu.SMEM)] * scalar
    specs += [whole()] * (len(operands) - scalar)
    shapes = [jax.ShapeDtypeStruct(shape, dtype) for shape, dtype in outs]
    return pl.pallas_call(
        kernel,
        in_specs=more.pop("in_specs", specs),
        out_specs=[pl.BlockSpec(memory_space=space)] * len(shapes),
        out_shape=shapes,
        scratch_shapes=scratch,
        compiler_params=pltpu.CompilerParams(vmem_limit_bytes=GRANT),
        cost_estimate=pl.CostEstimate(flops=flops, bytes_accessed=0, transcendentals=0),
        **more,
    )(*operands)


def fast_body(tokens, norm_gain, w_query, w_key, w_value, w_pool_in, sink_logit, pool_scale, w_out):
    sp_count, tp_count = lax.axis_size("sp"), lax.axis_size("tp")
    rows, width = tokens.shape
    heads_width, channels = w_query.shape[1], w_pool_in.shape[1]
    kv_orders, out_orders = exchange_orders(sp_count, tp_count)

    key_head = lax.axis_index("tp") * (heads_width // HEAD) // (QH // KVH)
    kv_block = jnp.concatenate(
        [lax.dynamic_slice_in_dim(w, key_head * HEAD, HEAD, 1) for w in (w_key, w_value)], axis=1
    )
    kv_pieces = doubled(kv_block, kv_orders, sp_count, tp_count, True)
    out_pieces = doubled(w_out, out_orders, sp_count, tp_count, False)

    base, blocks = (jnp.array(table) for table in rope_tables(rows * sp_count))
    edge = 2 * (POOL_SPANS[-1] // 2)
    inner = rows // 2 - QB
    scale = pool_scale[None, :]

    loaded = (tokens, norm_gain[None, :], w_query, w_pool_in, base, blocks)
    loaded = [pltpu.with_memory_space_constraint(part, pltpu.HBM) for part in loaded]
    normed, w_query, w_pool_in, base, blocks = call(
        norm_kernel,
        loaded,
        [(tokens.shape, BF16)] + [(part.shape, part.dtype) for part in loaded[2:]],
        [
            pltpu.VMEM(tokens.shape, BF16),
            pltpu.VMEM((1, width), F32),
            pltpu.SemaphoreType.DMA((5 + rows // ROW_TILE,)),
        ],
        2 * rows * width * heads_width,
        in_specs=[pl.BlockSpec(memory_space=pltpu.HBM)] * 6,
    )
    pool, pooled_given, pooled = call(
        functools.partial(pool_kernel, edge),
        (normed, w_pool_in, scale),
        [((rows, channels), BF16)] + [((inner, channels), BF16)] * 2,
        [],
        2 * rows * width * channels,
    )
    (query,) = call(
        query_kernel,
        (normed, w_query, base, blocks),
        [((rows, heads_width), BF16)],
        [],
        2 * rows * width * heads_width,
    )
    payload = (WINDOW + edge * (channels // LANES), LANES)
    key_value, first, second = call(
        functools.partial(key_value_kernel, kv_orders, tp_count),
        (*kv_pieces, normed, pool, base, blocks),
        [((rows, LANES), BF16), (payload, BF16), (payload, BF16)],
        [pltpu.VMEM((width, LANES), BF16)],
        2 * rows * width * LANES,
    )

    across = [(i, i ^ 1) for i in range(sp_count)]
    between = [(i, i + 1) for i in range(1, sp_count - 1, 2)]
    first = lax.ppermute(first, "sp", across)
    second = lax.ppermute(second, "sp", between + [(b, a) for a, b in between])

    flops = 4 * rows * 3 * WINDOW * LANES * (heads_width // HEAD)
    given, attended = call(
        inner_kernel,
        (sink_logit, query, key_value),
        [((inner, heads_width), BF16)] * 2,
        [pltpu.VMEM((rows, LANES), BF16)] * 2,
        flops,
        scalar=1,
    )
    edge_given, edges = call(
        functools.partial(outer_kernel, sp_count),
        (sink_logit, query, key_value, pool, scale, first, second),
        [((QB, heads_width + channels), BF16)] * 2,
        [],
        flops // 3,
        scalar=1,
    )
    other = [(0, 1), (1, 0)]
    pooled_came = lax.ppermute(pooled_given, "tp", other)
    attended_came = lax.ppermute(given, "tp", other)
    edges_came = lax.ppermute(edge_given, "tp", other)

    columns = w_out.shape[1] * sp_count
    tables = [
        (flip, output_tables(out_orders, late, tp_count)) for flip in range(2) for late in range(2)
    ]
    parts = (attended, pooled, edges, attended_came, pooled_came, edges_came)
    held, came, early, late = out_pieces
    flops = rows * columns * w_out.shape[0]
    staged = (sp_count // 4, rows // 2, w_out.shape[1])
    shape = (rows // 2, columns)
    in_hbm, in_vmem = pl.BlockSpec(memory_space=pltpu.HBM), whole()
    out, joined = pl.pallas_call(
        functools.partial(output_kernel, [tables[0], tables[2], tables[1]], True),
        in_specs=[in_vmem] * 9,
        out_specs=[in_hbm, in_vmem],
        out_shape=[
            jax.ShapeDtypeStruct(shape, BF16),
            jax.ShapeDtypeStruct((rows // 2, 2 * w_out.shape[0]), BF16),
        ],
        scratch_shapes=[
            pltpu.VMEM((3 * staged[0],) + staged[1:], BF16),
            pltpu.SemaphoreType.DMA((3 * staged[0],)),
        ],
        compiler_params=pltpu.CompilerParams(vmem_limit_bytes=GRANT),
        cost_estimate=pl.CostEstimate(flops=flops, bytes_accessed=0, transcendentals=0),
        name="output",
    )(held, early, came, *parts)
    return pl.pallas_call(
        functools.partial(output_kernel, [tables[3]], False),
        in_specs=[in_vmem, in_vmem, in_hbm],
        out_specs=in_hbm,
        out_shape=jax.ShapeDtypeStruct(shape, BF16),
        input_output_aliases={2: 0},
        scratch_shapes=[pltpu.VMEM(staged, BF16), pltpu.SemaphoreType.DMA((staged[0],))],
        compiler_params=pltpu.CompilerParams(vmem_limit_bytes=GRANT),
        cost_estimate=pl.CostEstimate(flops=flops // 3, bytes_accessed=0, transcendentals=0),
        name="finish",
    )(late, joined, out)


def tiled(rows, w_query, w_pool_in, w_out):
    sp_count, tp_count = lax.axis_size("sp"), lax.axis_size("tp")
    return (
        sp_count & (sp_count - 1) == 0
        and sp_count >= 8
        and tp_count == 2
        and rows % (2 * ROW_TILE) == 0
        and 2 * w_query.shape[1] == QH * HEAD
        and w_query.shape[1] == w_pool_in.shape[1]
        and w_pool_in.shape[1] % LANES == 0
        and w_out.shape[1] % LANES == 0
    )


def body(*args):
    tokens, w_query, w_pool_in, w_out = args[0], args[2], args[5], args[8]
    if tiled(tokens.shape[0], w_query, w_pool_in, w_out):
        return fast_body(*args)
    return plain_body(*args)


def solution(mesh):
    in_specs = (
        P("sp", None),
        P(),
        P(None, "tp"),
        P("sp", None),
        P("sp", None),
        P(None, "tp"),
        P("tp"),
        P("tp"),
        P("tp", "sp"),
    )
    out_specs = P(("sp", "tp"), None)
    return jax.shard_map(body, mesh=mesh, in_specs=in_specs, out_specs=out_specs, check_vma=False)
```
